32 devices in a mesh: dp: 4 (over y, x), kv: 4 (over z), tp: 2 (over core).
Axes of the slice: x: 2, y: 2, z: 4, core: 2. Of those that a mesh axis runs over, the one named last changes fastest.
Arguments:
- tokens: bfloat16 [1024, 2048], P(('dp', 'kv', 'tp')), may hold values from -6 to 6
- norm_gain: float32 [2048], replicated, may hold values from 0.1 to 1.9
- gate_proj: bfloat16 [2048, 4096], P(None, ('kv', 'tp')), may hold values from -0.125 to 0.125
- inner_proj: bfloat16 [2048, 4096], P(None, ('kv', 'tp')), may hold values from -0.125 to 0.125
- write_proj: bfloat16 [2048, 1024], P(None, ('kv', 'tp')), may hold values from -0.125 to 0.125
- read_proj: bfloat16 [2048, 1024], P(None, ('kv', 'tp')), may hold values from -0.125 to 0.125
- step_proj: bfloat16 [2048, 64], replicated, may hold values from -0.125 to 0.125
- step_bias: float32 [64], replicated, may hold values from -3 to 0
- decay_log: float32 [64], replicated, may hold values from -5 to 0.7
- skip_gain: float32 [64], replicated, may hold values from 0.25 to 4
- conv_inner: bfloat16 [4, 4096], replicated, may hold values from -3 to 3
- conv_write: bfloat16 [4, 1024], replicated, may hold values from -3 to 3
- conv_read: bfloat16 [4, 1024], replicated, may hold values from -3 to 3
- out_gain: float32 [4096], replicated, may hold values from 0.1 to 1.9
- out_proj: bfloat16 [4096, 2048], P(('kv', 'tp')), may hold values from -0.09375 to 0.09375
- saved_state: float32 [256, 64, 64, 128], P('dp', ('kv', 'tp')), may hold values from -1.75 to 1.75
- inner_history: bfloat16 [256, 7, 4096], P('dp', None, ('kv', 'tp')), may hold values from -6 to 6
- write_history: bfloat16 [256, 7, 1024], P('dp', None, ('kv', 'tp')), may hold values from -6 to 6
- read_history: bfloat16 [256, 7, 1024], P('dp', None, ('kv', 'tp')), may hold values from -6 to 6
- last_steps: float32 [256, 4, 64], P('dp', None, ('kv', 'tp')), may hold values from 0.02 to 1
- accepted: int32 [256], P('dp'), may hold values from 0 to 4
Outputs:
- mixed: bfloat16 [1024, 2048], P(('dp', 'kv', 'tp'))
- base_state: float32 [256, 64, 64, 128], P('dp', ('kv', 'tp'))
The draws below stay inside these ranges and needn't reach their ends.
All inputs are finite; a program needn't handle non-finite values.
Results may differ from the reference program's by a relative error of at most 0.014.
Values may be sent and summed in bfloat16 or wider, within the bound.
A program may use at most 128 MiB of HBM per device.

```python
import math
import jax
import jax.numpy as jnp
from jax import lax

D = 2048
HEADS = 64
HEAD_DIM = 64
STATE = 128
GROUPS = 8
WIDTH = 4
PROP = 4
INNER = 4096
SEQS = 256
TOKENS = 1024
HIST = 7


def draw_decay_log(key, part):
    spread_draw = jax.random.uniform(key, (HEADS,), jnp.float32)
    return -3.9 + 4.6 * spread_draw


def touch_ends(array, rng, least, largest):
    longest = array.shape.index(max(array.shape))
    spots = []
    for shift in (0, 1):
        where = [jax.random.randint(jax.random.fold_in(rng, axis), (), 0, length) for axis, length in enumerate(array.shape)]
        where[longest] = (where[longest] + shift) % array.shape[longest]
        spots.append(tuple(where))
    return array.at[spots[0]].set(least).at[spots[1]].set(largest)


def steps_of(rng, dims, pieces, low, high):
    factor_of = 1.0
    for axis_at, shards_of in pieces:
        draws = jax.random.uniform(jax.random.fold_in(jax.random.fold_in(rng, 6), axis_at), (shards_of,), jnp.float32, low / len(pieces), high / len(pieces))
        factor_of = factor_of * jnp.repeat(jnp.exp(draws), dims[axis_at] // shards_of).reshape((-1,) + (1,) * (len(dims) - 1 - axis_at))
    return factor_of


def normal_values(stream_key, extent, width, reach, shards=(), kind=jnp.bfloat16):
    factor_of = steps_of(stream_key, extent, shards, -0.22, 0.18) if shards else 1.0
    array = jax.random.normal(stream_key, extent, jnp.float32) * width * factor_of
    return jnp.minimum(jnp.maximum(array, -reach), reach).astype(kind)


def setup_inputs(seed: int = 0) -> dict:
    key_list = jax.random.split(jax.random.key(seed), 22)
    tokens = normal_values(key_list[0], (TOKENS, D), 1.0, 6.0, ((0, 32),))
    norm_gain = jnp.clip(1.0 + 0.18 * jax.random.normal(key_list[1], (D,), jnp.float32), 0.1, 1.9)
    gate_proj = normal_values(key_list[2], (D, INNER), D ** -0.5, 0.125, ((1, 8),))
    inner_proj = normal_values(key_list[3], (D, INNER), D ** -0.5, 0.125, ((1, 8),))
    write_proj = normal_values(key_list[4], (D, GROUPS * STATE), D ** -0.5, 0.125, ((1, 8),))
    read_proj = normal_values(key_list[5], (D, GROUPS * STATE), D ** -0.5, 0.125, ((1, 8),))
    step_proj = normal_values(key_list[6], (D, HEADS), D ** -0.5, 0.125)
    step_bias = jnp.clip(jax.random.uniform(key_list[7], (HEADS,), jnp.float32, -3.0, 0.0), -3.0, 0.0)
    decay_log = draw_decay_log(jax.random.fold_in(key_list[21], 71), 0)
    skip_gain = jnp.clip(jnp.exp(jax.random.uniform(key_list[9], (HEADS,), jnp.float32, math.log(0.25), math.log(4.0))), 0.25, 4.0)
    conv_inner = normal_values(key_list[10], (WIDTH, INNER), WIDTH ** -0.5, 3.0)
    conv_write = normal_values(key_list[11], (WIDTH, GROUPS * STATE), WIDTH ** -0.5, 3.0)
    conv_read = normal_values(key_list[12], (WIDTH, GROUPS * STATE), WIDTH ** -0.5, 3.0)
    out_gain = jnp.clip(1.0 + 0.18 * jax.random.normal(key_list[13], (INNER,), jnp.float32), 0.1, 1.9)
    out_proj = normal_values(key_list[14], (INNER, D), INNER ** -0.5, 0.09375, ((0, 8),))
    saved_state = normal_values(key_list[15], (SEQS, HEADS, HEAD_DIM, STATE), 0.3, 1.75, ((0, 4), (1, 8)), jnp.float32)
    inner_history = normal_values(key_list[16], (SEQS, HIST, INNER), 1.0, 6.0, ((0, 4), (2, 8)))
    write_history = normal_values(key_list[17], (SEQS, HIST, GROUPS * STATE), 1.0, 6.0, ((0, 4), (2, 8)))
    read_history = normal_values(key_list[18], (SEQS, HIST, GROUPS * STATE), 1.0, 6.0, ((0, 4), (2, 8)))
    last_steps = jnp.clip(jnp.exp(math.log(1.0) - 3.912023 * jax.random.uniform(key_list[19], (SEQS, PROP, HEADS), jnp.float32) ** steps_of(key_list[19], (SEQS, PROP, HEADS), ((0, 4), (2, 8)), -0.2, 0.2)), 0.02, 1.0)
    accepted = touch_ends(jax.random.randint(key_list[20], (SEQS,), 0, PROP + 1), jax.random.fold_in(key_list[20], 1), 0, PROP).astype(jnp.int32)
    return {"tokens": tokens, "norm_gain": norm_gain, "gate_proj": gate_proj, "inner_proj": inner_proj, "write_proj": write_proj, "read_proj": read_proj, "step_proj": step_proj, "step_bias": step_bias, "decay_log": decay_log, "skip_gain": skip_gain, "conv_inner": conv_inner, "conv_write": conv_write, "conv_read": conv_read, "out_gain": out_gain, "out_proj": out_proj, "saved_state": saved_state, "inner_history": inner_history, "write_history": write_history, "read_history": read_history, "last_steps": last_steps, "accepted": accepted}


EPSILON = 0.1
highest = lax.Precision.HIGHEST

def conv_rows(row_block, weight):
    out_len = row_block.shape[1] - weight.shape[0] + 1
    result = weight[0] * row_block[:, 0:out_len]
    for offset in range(1, weight.shape[0]):
        result = result + weight[offset] * row_block[:, offset:offset + out_len]
    return result

def rounded(values):
    return lax.optimization_barrier(values.astype(jnp.bfloat16)).astype(jnp.float32)

def reference(tokens, norm_gain, gate_proj, inner_proj, write_proj, read_proj, step_proj, step_bias, decay_log, skip_gain, conv_inner, conv_write, conv_read, out_gain, out_proj, saved_state, inner_history, write_history, read_history, last_steps, accepted):
    seq_count = saved_state.shape[0]
    own_rows = tokens.astype(jnp.float32)
    normed = (own_rows * lax.rsqrt(lax.optimization_barrier(jnp.mean(own_rows * own_rows, axis=-1, keepdims=True)) + EPSILON) * norm_gain).astype(jnp.bfloat16)
    gate_rows = jnp.dot(normed, gate_proj, preferred_element_type=jnp.float32).astype(jnp.bfloat16)
    inner_rows = jnp.dot(normed, inner_proj, preferred_element_type=jnp.float32).astype(jnp.bfloat16)
    write_rows = jnp.dot(normed, write_proj, preferred_element_type=jnp.float32).astype(jnp.bfloat16)
    read_rows = jnp.dot(normed, read_proj, preferred_element_type=jnp.float32).astype(jnp.bfloat16)
    step_rows = jnp.dot(normed, step_proj, preferred_element_type=jnp.float32)
    conv_width = conv_inner.shape[0]
    window_rows = (accepted[:, None] + jnp.arange(conv_width - 1, dtype=jnp.int32)[None, :]).astype(jnp.int32)

    def current(history, new_rows, weight):
        window = jnp.take_along_axis(history, window_rows[:, :, None], axis=1)
        joined = jnp.concatenate([window, new_rows.reshape(seq_count, PROP, -1)], axis=1)
        return jax.nn.silu(conv_rows(joined.astype(jnp.float32), weight.astype(jnp.float32)))
    inner_old = jax.nn.silu(conv_rows(inner_history.astype(jnp.float32), conv_inner.astype(jnp.float32)))
    write_old = rounded(jax.nn.silu(conv_rows(write_history.astype(jnp.float32), conv_write.astype(jnp.float32))))
    inner_new = current(inner_history, inner_rows, conv_inner)
    write_new = rounded(current(write_history, write_rows, conv_write))
    read_new = rounded(current(read_history, read_rows, conv_read))
    step_size = jax.nn.softplus(step_rows + step_bias[None, :]).reshape(seq_count, PROP, HEADS)
    decay_rate = -jnp.exp(decay_log)
    per_group = HEADS // GROUPS
    accepted_mask = (jnp.arange(PROP, dtype=jnp.int32)[None, :] < accepted[:, None]).astype(jnp.float32)
    step_logs = decay_rate[None, None, :] * last_steps * accepted_mask[:, :, None]
    total_log = lax.optimization_barrier(jnp.sum(step_logs, axis=1))
    tail_log = total_log[:, None, :] - jnp.cumsum(step_logs, axis=1)
    old_weights = accepted_mask[:, :, None] * jnp.exp(tail_log) * last_steps
    inner_old_heads = inner_old.reshape(seq_count, PROP, HEADS, HEAD_DIM)
    write_old_heads = jnp.repeat(write_old.reshape(seq_count, PROP, GROUPS, STATE), per_group, axis=2)
    base_state = jnp.exp(total_log)[:, :, None, None] * saved_state + jnp.einsum('sth,sthp,sthn->shpn', old_weights, inner_old_heads, write_old_heads, precision=highest)
    cumulative = jnp.cumsum(decay_rate[None, None, :] * step_size, axis=1)
    log_gap = cumulative[:, :, None, :] - cumulative[:, None, :, :]
    causal = (jnp.arange(PROP)[:, None] >= jnp.arange(PROP)[None, :])[None, :, :, None]
    kernel = jnp.where(causal, jnp.exp(jnp.where(causal, log_gap, 0.0)), 0.0)
    write_heads = jnp.repeat(write_new.reshape(seq_count, PROP, GROUPS, STATE), per_group, axis=2)
    read_heads = jnp.repeat(read_new.reshape(seq_count, PROP, GROUPS, STATE), per_group, axis=2)
    scores = jnp.einsum('sihn,sjhn->sijh', read_heads, write_heads, precision=highest)
    inner_heads = inner_new.reshape(seq_count, PROP, HEADS, HEAD_DIM)
    within = jnp.einsum('sijh,sjh,sjhp->sihp', kernel * scores, step_size, inner_heads, precision=highest)
    carried = jnp.exp(cumulative)[..., None] * jnp.einsum('sihn,shpn->sihp', read_heads, base_state, precision=highest)
    mixed_heads = within + carried + skip_gain[None, None, :, None] * inner_heads
    gated_rows = mixed_heads.reshape(seq_count * PROP, INNER) * jax.nn.silu(gate_rows.astype(jnp.float32))
    squares = lax.optimization_barrier(jnp.mean(gated_rows * gated_rows, axis=-1, keepdims=True))
    unscaled = (gated_rows * out_gain).astype(jnp.bfloat16)
    mixed = (jnp.dot(unscaled, out_proj, preferred_element_type=jnp.float32) * lax.rsqrt(squares + EPSILON)).astype(jnp.bfloat16)
    return (mixed, base_state)
```

```python
import functools

import jax
import jax.numpy as jnp
from jax import lax
from jax.experimental import pallas as pl
from jax.experimental.pallas import tpu as pltpu
from jax.sharding import PartitionSpec as P

GROUPS = 8
EPSILON = 0.1
BLOCK = 8
highest = lax.Precision.HIGHEST


def swapped(value, axis, stride):
    mask = 2**stride
    pairs = [(source, source ^ mask) for source in range(lax.axis_size(axis))]
    return lax.ppermute(value, axis, pairs)


def mix_kernel(
    rank_ref,
    acc_ref,
    steps_ref,
    last_ref,
    par_ref,
    gate_ref,
    inner_ref,
    write_ref,
    read_ref,
    hist_inner_ref,
    hist_write_ref,
    hist_read_ref,
    taps_inner_ref,
    taps_write_ref,
    taps_read_ref,
    gain_ref,
    expand_ref,
    state_ref,
    un_ref,
    sq_ref,
    base_ref,
):
    f32 = jnp.float32
    props = steps_ref.shape[0]
    heads = steps_ref.shape[2]
    cols = inner_ref.shape[2]
    states = write_ref.shape[2]
    head_dim = cols // heads
    hist = hist_inner_ref.shape[0]
    width = taps_inner_ref.shape[0]
    acc = acc_ref[...]

    def silu(x):
        return x / (1.0 + jnp.exp(-x))

    def slabs(ref):
        return [ref[k].astype(f32) for k in range(ref.shape[0])]

    def conv(rows, taps_ref):
        taps = taps_ref[...].astype(f32)
        res = []
        for r in range(len(rows) - width + 1):
            v = taps[0:1] * rows[r]
            for k in range(1, width):
                v = v + taps[k : k + 1] * rows[r + k]
            res.append(silu(v))
        return res

    def current(h, new_ref):
        where_at = jnp.broadcast_to(acc, h[0].shape)
        rows = []
        for k in range(width - 1):
            r = h[k]
            for v in range(1, hist - width + 2):
                r = jnp.where(where_at == v, h[k + v], r)
            rows.append(r)
        return rows + slabs(new_ref)

    h_inner = slabs(hist_inner_ref)
    inner_old = conv(h_inner, taps_inner_ref)
    inner_new = conv(current(h_inner, inner_ref), taps_inner_ref)
    h_write = slabs(hist_write_ref)
    round_bf = lambda x: x.astype(jnp.bfloat16).astype(f32)
    write_old = [round_bf(x) for x in conv(h_write, taps_write_ref)]
    write_new = [round_bf(x) for x in conv(current(h_write, write_ref), taps_write_ref)]
    read_new = [round_bf(x) for x in conv(current(slabs(hist_read_ref), read_ref), taps_read_ref)]

    bias = par_ref[0:1]
    rate = -jnp.exp(par_ref[1:2])
    skip = par_ref[2:3]
    acc_h = jnp.broadcast_to(acc, (BLOCK, heads))
    masks = [jnp.where(acc_h > t, 1.0, 0.0) for t in range(props)]
    logs = [rate * last_ref[t] * masks[t] for t in range(props)]
    coefs = [None] * props
    tail = jnp.zeros((BLOCK, heads), f32)
    for t in reversed(range(props)):
        coefs[t] = masks[t] * jnp.exp(tail) * last_ref[t]
        tail = tail + logs[t]
    decay = jnp.exp(tail)
    step = []
    for t in range(props):
        x = steps_ref[t] + bias
        step.append(jnp.maximum(x, 0.0) + jnp.log1p(jnp.exp(-jnp.abs(x))))
    cums = []
    for t in range(props):
        cums.append(rate * step[t] + (cums[-1] if cums else 0.0))
    where_of = {}
    for i in range(props):
        for j in range(i + 1):
            score = jnp.sum(read_new[i] * write_new[j], axis=-1, keepdims=True)
            c = jnp.exp(cums[i] - cums[j]) * step[j] * score
            if i == j:
                c = c + skip
            where_of[(i, j)] = len(coefs)
            coefs.append(c)
    first_cum = len(coefs)
    for i in range(props):
        coefs.append(jnp.exp(cums[i]))
    wide = jnp.dot(
        jnp.concatenate(coefs, axis=0),
        expand_ref[...],
        precision=highest,
        preferred_element_type=f32,
    )

    def at(k):
        return wide[k * BLOCK : (k + 1) * BLOCK]

    left = jnp.concatenate([at(t) * inner_old[t] for t in range(props)], axis=0)
    high = round_bf(left)
    both = jnp.concatenate([high, left - high], axis=0)
    turned = jnp.transpose(both).astype(jnp.bfloat16)
    write_all = jnp.concatenate(write_old + write_old, axis=0)
    read_all = jnp.concatenate(read_new, axis=0)
    seq_w = lax.broadcasted_iota(jnp.int32, write_all.shape, 0) % BLOCK
    seq_r = lax.broadcasted_iota(jnp.int32, read_all.shape, 0) % BLOCK
    carried = jnp.zeros((props * BLOCK, cols), f32)
    for s in range(BLOCK):
        right = jnp.where(seq_w == s, write_all, 0.0).astype(jnp.bfloat16)
        update = jnp.dot(turned, right, preferred_element_type=f32)
        parts = []
        for h in range(heads):
            lo, hi = h * head_dim, (h + 1) * head_dim
            d = jnp.broadcast_to(decay[s : s + 1, h : h + 1], (head_dim, states))
            new = d * state_ref[s, lo:hi, :] + update[lo:hi]
            base_ref[s, lo:hi, :] = new
            parts.append(new.astype(jnp.bfloat16))
        asked = jnp.where(seq_r == s, read_all, 0.0).astype(jnp.bfloat16)
        carried = carried + lax.dot_general(
            asked,
            jnp.concatenate(parts, axis=0),
            (((1,), (1,)), ((), ())),
            preferred_element_type=f32,
        )
    for i in range(props):
        y = at(first_cum + i) * carried[i * BLOCK : (i + 1) * BLOCK]
        for j in range(i + 1):
            y = y + at(where_of[(i, j)]) * inner_new[j]
        g = y * silu(gate_ref[i].astype(f32))
        sq_ref[i] = jnp.broadcast_to(jnp.sum(g * g, axis=-1, keepdims=True), sq_ref.shape[1:])
        un_ref[i] = (g * gain_ref[...]).astype(un_ref.dtype)


def mix(rank, group, acc, steps, last, par, gate, inner, write, read, hi, hw, hr, ci, cw, cr, gain, state):
    props, seqs, heads = steps.shape
    cols, states = state.shape[1], state.shape[2]
    expand = (jnp.arange(cols)[None, :] // (cols // heads) == jnp.arange(heads)[:, None]).astype(
        jnp.float32
    )
    hist = hi.shape[0]
    width = ci.shape[0]

    def slab(lead, last_dim):
        return pl.BlockSpec((lead, BLOCK, last_dim), lambda g, r: (0, g, 0))

    def own(rows, last_dim, which):
        return pl.BlockSpec((rows, last_dim), lambda g, r: (0, r[which]))

    state_spec = pl.BlockSpec((BLOCK, cols, states), lambda g, r: (g, 0, 0))
    return pl.pallas_call(
        mix_kernel,
        grid_spec=pltpu.PrefetchScalarGridSpec(
            num_scalar_prefetch=1,
            grid=(seqs // BLOCK,),
            in_specs=[
                pl.BlockSpec((BLOCK, 1), lambda g, r: (g, 0)),
                slab(props, heads),
                slab(props, heads),
                pl.BlockSpec(par.shape, lambda g, r: (0, 0)),
                slab(props, cols),
                slab(props, cols),
                slab(props, states),
                slab(props, states),
                slab(hist, cols),
                slab(hist, states),
                slab(hist, states),
                own(width, cols, 0),
                own(width, states, 1),
                own(width, states, 1),
                own(1, cols, 0),
                pl.BlockSpec(expand.shape, lambda g, r: (0, 0)),
                state_spec,
            ],
            out_specs=[slab(props, cols), slab(props, 128), state_spec],
        ),
        out_shape=[
            jax.ShapeDtypeStruct((props, seqs, cols), jnp.bfloat16),
            jax.ShapeDtypeStruct((props, seqs, 128), jnp.float32),
            jax.ShapeDtypeStruct(state.shape, jnp.float32),
        ],
        compiler_params=pltpu.CompilerParams(
            dimension_semantics=("arbitrary",), vmem_limit_bytes=48 * 1024 * 1024
        ),
        name="mix",
    )(
        jnp.stack([rank, group]).astype(jnp.int32),
        acc, steps, last, par, gate, inner, write, read, hi, hw, hr, ci, cw, cr, gain, expand, state,
    )


def gathered(own):
    return lax.all_gather(own, ("kv", "tp"), axis=0, tiled=True)


def body(
    tokens,
    norm_gain,
    gate_proj,
    inner_proj,
    write_proj,
    read_proj,
    step_proj,
    step_bias,
    decay_log,
    skip_gain,
    conv_inner,
    conv_write,
    conv_read,
    out_gain,
    out_proj,
    saved_state,
    inner_history,
    write_history,
    read_history,
    last_steps,
    accepted,
):
    device_rank = lax.axis_index(("kv", "tp"))
    seq_count = saved_state.shape[0]
    local_heads = saved_state.shape[1]
    head_dim = saved_state.shape[2]
    proposals = last_steps.shape[1]
    inner_cols = inner_proj.shape[1]
    state_cols = write_proj.shape[1]
    token_count = tokens.shape[0]
    own_rows = tokens.astype(jnp.float32)
    normed_own = (
        own_rows
        * lax.rsqrt(jnp.mean(own_rows * own_rows, axis=-1, keepdims=True) + EPSILON)
        * norm_gain
    ).astype(jnp.bfloat16)
    normed = gathered(normed_own)
    normed = normed.reshape(seq_count, proposals, -1).transpose(1, 0, 2)
    normed = normed.reshape(proposals * seq_count, -1)

    def project(weight):
        out = jnp.dot(normed, weight, preferred_element_type=jnp.float32)
        return out.reshape(proposals, seq_count, -1)

    gate_rows = project(gate_proj).astype(jnp.bfloat16)
    inner_rows = project(inner_proj).astype(jnp.bfloat16)
    write_rows = project(write_proj).astype(jnp.bfloat16)
    read_rows = project(read_proj).astype(jnp.bfloat16)
    first_head = device_rank * local_heads
    steps = lax.dynamic_slice_in_dim(project(step_proj), first_head, local_heads, 2)
    par = lax.dynamic_slice_in_dim(
        jnp.stack([step_bias, decay_log, skip_gain]), first_head, local_heads, 1
    )
    slab = lambda x: x.transpose(1, 0, 2)
    hist_inner, hist_write, hist_read = slab(inner_history), slab(write_history), slab(read_history)
    pieces = (write_rows, read_rows, hist_write, hist_read)
    group_span = lax.axis_size("kv") * lax.axis_size("tp") // GROUPS
    if group_span >= 2:
        pieces = tuple(lax.all_gather(x, "tp", axis=2, tiled=True) for x in pieces)
        kv_rank = lax.axis_index("kv")
        bit_count = (group_span // lax.axis_size("tp")).bit_length() - 1
        for bit in range(bit_count):
            partner = swapped(pieces, "kv", bit)
            lower = jnp.bitwise_and(jnp.right_shift(kv_rank, bit), 1) == 0
            pieces = tuple(
                jnp.where(
                    lower,
                    jnp.concatenate([mine, theirs], axis=2),
                    jnp.concatenate([theirs, mine], axis=2),
                )
                for mine, theirs in zip(pieces, partner)
            )
    write_rows, read_rows, hist_write, hist_read = pieces
    unscaled, squares, base_state = mix(
        device_rank,
        device_rank // group_span,
        accepted[:, None],
        steps,
        slab(last_steps),
        par,
        gate_rows,
        inner_rows,
        write_rows,
        read_rows,
        hist_inner,
        hist_write,
        hist_read,
        conv_inner,
        conv_write,
        conv_read,
        out_gain[None, :],
        saved_state.reshape(seq_count, local_heads * head_dim, -1),
    )
    base_state = base_state.reshape(saved_state.shape)
    unscaled = unscaled.transpose(1, 0, 2).reshape(seq_count * proposals, inner_cols)
    partial_value = jnp.dot(unscaled, out_proj, preferred_element_type=jnp.float32)
    squares = squares[:, :, 0].T.reshape(-1)
    square_total = lax.psum(squares, ("kv", "tp"))
    summed = lax.psum_scatter(partial_value, ("kv", "tp"), scatter_dimension=0, tiled=True)
    square_own = lax.dynamic_slice_in_dim(square_total, device_rank * token_count, token_count, 0)
    mixed = (summed * lax.rsqrt(square_own / out_gain.shape[0] + EPSILON)[:, None]).astype(jnp.bfloat16)
    return (mixed, base_state)


def solution(mesh):
    placed = (
        P(("dp", "kv", "tp"), None),
        P(),
        P(None, ("kv", "tp")),
        P(None, ("kv", "tp")),
        P(None, ("kv", "tp")),
        P(None, ("kv", "tp")),
        P(),
        P(),
        P(),
        P(),
        P(),
        P(),
        P(),
        P(),
        P(("kv", "tp"), None),
        P("dp", ("kv", "tp"), None, None),
        P("dp", None, ("kv", "tp")),
        P("dp", None, ("kv", "tp")),
        P("dp", None, ("kv", "tp")),
        P("dp", None, ("kv", "tp")),
        P("dp"),
    )
    return jax.shard_map(
        body,
        mesh=mesh,
        in_specs=placed,
        out_specs=(P(("dp", "kv", "tp"), None), P("dp", ("kv", "tp"), None, None)),
        check_vma=False,
    )
```

```python
import functools

import jax
import jax.numpy as jnp
from jax import lax
from jax.experimental import pallas as pl
from jax.experimental.pallas import tpu as pltpu
from jax.sharding import PartitionSpec as P

GROUPS = 8
EPSILON = 0.1
BLOCK = 8
highest = lax.Precision.HIGHEST


def swapped(value, axis, stride):
    mask = 2**stride
    pairs = [(source, source ^ mask) for source in range(lax.axis_size(axis))]
    return lax.ppermute(value, axis, pairs)


def mix_kernel(
    rank_ref,
    acc_ref,
    steps_ref,
    last_ref,
    par_ref,
    gate_ref,
    inner_ref,
    write_ref,
    read_ref,
    hist_inner_ref,
    hist_write_ref,
    hist_read_ref,
    taps_inner_ref,
    taps_write_ref,
    taps_read_ref,
    gain_ref,
    expand_ref,
    state_ref,
    un_ref,
    sq_ref,
    base_ref,
):
    f32 = jnp.float32
    props = steps_ref.shape[0]
    heads = steps_ref.shape[2]
    cols = inner_ref.shape[2]
    states = write_ref.shape[2]
    head_dim = cols // heads
    hist = hist_inner_ref.shape[0]
    width = taps_inner_ref.shape[0]
    acc = acc_ref[...]

    def silu(x):
        return x / (1.0 + jnp.exp(-x))

    def slabs(ref):
        return [ref[k].astype(f32) for k in range(ref.shape[0])]

    def conv(rows, taps_ref):
        taps = taps_ref[...].astype(f32)
        res = []
        for r in range(len(rows) - width + 1):
            v = taps[0:1] * rows[r]
            for k in range(1, width):
                v = v + taps[k : k + 1] * rows[r + k]
            res.append(silu(v))
        return res

    def current(h, new_ref):
        where_at = jnp.broadcast_to(acc, h[0].shape)
        rows = []
        for k in range(width - 1):
            r = h[k]
            for v in range(1, hist - width + 2):
                r = jnp.where(where_at == v, h[k + v], r)
            rows.append(r)
        return rows + slabs(new_ref)

    h_inner = slabs(hist_inner_ref)
    inner_old = conv(h_inner, taps_inner_ref)
    inner_new = conv(current(h_inner, inner_ref), taps_inner_ref)
    h_write = slabs(hist_write_ref)
    round_bf = lambda x: x.astype(jnp.bfloat16).astype(f32)
    write_old = [round_bf(x) for x in conv(h_write, taps_write_ref)]
    write_new = [round_bf(x) for x in conv(current(h_write, write_ref), taps_write_ref)]
    read_new = [round_bf(x) for x in conv(current(slabs(hist_read_ref), read_ref), taps_read_ref)]

    bias = par_ref[0:1]
    rate = -jnp.exp(par_ref[1:2])
    skip = par_ref[2:3]
    acc_h = jnp.broadcast_to(acc, (BLOCK, heads))
    masks = [jnp.where(acc_h > t, 1.0, 0.0) for t in range(props)]
    logs = [rate * last_ref[t] * masks[t] for t in range(props)]
    coefs = [None] * props
    tail = jnp.zeros((BLOCK, heads), f32)
    for t in reversed(range(props)):
        coefs[t] = masks[t] * jnp.exp(tail) * last_ref[t]
        tail = tail + logs[t]
    decay = jnp.exp(tail)
    step = []
    for t in range(props):
        x = steps_ref[t] + bias
        step.append(jnp.maximum(x, 0.0) + jnp.log1p(jnp.exp(-jnp.abs(x))))
    cums = []
    for t in range(props):
        cums.append(rate * step[t] + (cums[-1] if cums else 0.0))
    where_of = {}
    for i in range(props):
        for j in range(i + 1):
            score = jnp.sum(read_new[i] * write_new[j], axis=-1, keepdims=True)
            c = jnp.exp(cums[i] - cums[j]) * step[j] * score
            if i == j:
                c = c + skip
            where_of[(i, j)] = len(coefs)
            coefs.append(c)
    first_cum = len(coefs)
    for i in range(props):
        coefs.append(jnp.exp(cums[i]))
    wide = jnp.dot(
        jnp.concatenate(coefs, axis=0),
        expand_ref[...],
        precision=highest,
        preferred_element_type=f32,
    )

    def at(k):
        return wide[k * BLOCK : (k + 1) * BLOCK]

    left = jnp.concatenate([at(t) * inner_old[t] for t in range(props)], axis=0)
    high = round_bf(left)
    both = jnp.concatenate([high, left - high], axis=0)
    turned = jnp.transpose(both).astype(jnp.bfloat16)
    write_all = jnp.concatenate(write_old + write_old, axis=0)
    read_all = jnp.concatenate(read_new, axis=0)
    seq_w = lax.broadcasted_iota(jnp.int32, write_all.shape, 0) % BLOCK
    seq_r = lax.broadcasted_iota(jnp.int32, read_all.shape, 0) % BLOCK
    carried = jnp.zeros((props * BLOCK, cols), f32)
    for s in range(BLOCK):
        right = jnp.where(seq_w == s, write_all, 0.0).astype(jnp.bfloat16)
        update = jnp.dot(turned, right, preferred_element_type=f32)
        parts = []
        for h in range(heads):
            lo, hi = h * head_dim, (h + 1) * head_dim
            d = jnp.broadcast_to(decay[s : s + 1, h : h + 1], (head_dim, states))
            new = d * state_ref[s, lo:hi, :] + update[lo:hi]
            base_ref[s, lo:hi, :] = new
            parts.append(new.astype(jnp.bfloat16))
        asked = jnp.where(seq_r == s, read_all, 0.0).astype(jnp.bfloat16)
        carried = carried + lax.dot_general(
            asked,
            jnp.concatenate(parts, axis=0),
            (((1,), (1,)), ((), ())),
            preferred_element_type=f32,
        )
    for i in range(props):
        y = at(first_cum + i) * carried[i * BLOCK : (i + 1) * BLOCK]
        for j in range(i + 1):
            y = y + at(where_of[(i, j)]) * inner_new[j]
        g = y * silu(gate_ref[i].astype(f32))
        sq_ref[i] = jnp.broadcast_to(jnp.sum(g * g, axis=-1, keepdims=True), sq_ref.shape[1:])
        un_ref[i] = (g * gain_ref[...]).astype(un_ref.dtype)


def mix(rank, group, acc, steps, last, par, gate, inner, write, read, hi, hw, hr, ci, cw, cr, gain, state):
    props, seqs, heads = steps.shape
    cols, states = state.shape[1], state.shape[2]
    expand = (jnp.arange(cols)[None, :] // (cols // heads) == jnp.arange(heads)[:, None]).astype(
        jnp.float32
    )
    hist = hi.shape[0]
    width = ci.shape[0]

    def slab(lead, last_dim):
        return pl.BlockSpec((lead, BLOCK, last_dim), lambda g, r: (0, g, 0))

    def own(rows, last_dim, which):
        return pl.BlockSpec((rows, last_dim), lambda g, r: (0, r[which]))

    state_spec = pl.BlockSpec((BLOCK, cols, states), lambda g, r: (g, 0, 0))
    return pl.pallas_call(
        mix_kernel,
        grid_spec=pltpu.PrefetchScalarGridSpec(
            num_scalar_prefetch=1,
            grid=(seqs // BLOCK,),
            in_specs=[
                pl.BlockSpec((BLOCK, 1), lambda g, r: (g, 0)),
                slab(props, heads),
                slab(props, heads),
                pl.BlockSpec(par.shape, lambda g, r: (0, 0)),
                slab(props, cols),
                slab(props, cols),
                slab(props, states),
                slab(props, states),
                slab(hist, cols),
                slab(hist, states),
                slab(hist, states),
                own(width, cols, 0),
                own(width, states, 1),
                own(width, states, 1),
                own(1, cols, 0),
                pl.BlockSpec(expand.shape, lambda g, r: (0, 0)),
                state_spec,
            ],
            out_specs=[slab(props, cols), slab(props, 128), state_spec],
        ),
        out_shape=[
            jax.ShapeDtypeStruct((props, seqs, cols), jnp.bfloat16),
            jax.ShapeDtypeStruct((props, seqs, 128), jnp.float32),
            jax.ShapeDtypeStruct(state.shape, jnp.float32),
        ],
        compiler_params=pltpu.CompilerParams(
            dimension_semantics=("arbitrary",), vmem_limit_bytes=48 * 1024 * 1024
        ),
        name="mix",
    )(
        jnp.stack([rank, group]).astype(jnp.int32),
        acc, steps, last, par, gate, inner, write, read, hi, hw, hr, ci, cw, cr, gain, expand, state,
    )


MESH = pl.DeviceIdType.MESH
CHUNKS = 2


def remote(src, dst, send, recv, where):
    return pltpu.make_async_remote_copy(
        src_ref=src, dst_ref=dst, send_sem=send, recv_sem=recv, device_id=where, device_id_type=MESH
    )


def gather_kernel(n, own_ref, out_ref, rs, rr, ls, lr, fs, fr, local_sem):
    k = lax.axis_index("kv")
    t = lax.axis_index("tp")
    right = {"kv": lax.rem(k + 1, n)}
    left = {"kv": lax.rem(k + n - 1, n)}
    partner = {"tp": 1 - t}
    span = own_ref.shape[1] // CHUNKS
    barrier = pltpu.get_barrier_semaphore()
    pl.semaphore_signal(barrier, inc=1, device_id=partner, device_id_type=MESH)

    @pl.when(k < n - 1)
    def _():
        pl.semaphore_signal(barrier, inc=1, device_id=right, device_id_type=MESH)

    @pl.when(k > 0)
    def _():
        pl.semaphore_signal(barrier, inc=1, device_id=left, device_id_type=MESH)

    inner = (k > 0) & (k < n - 1)

    @pl.when(inner)
    def _():
        pl.semaphore_wait(barrier, 3)

    @pl.when(jnp.logical_not(inner))
    def _():
        pl.semaphore_wait(barrier, 2)

    def view(j, c):
        return out_ref.at[j, t, :, pl.ds(c * span, span)]

    def own(c):
        return own_ref.at[:, pl.ds(c * span, span)]

    def to_right(s, c):
        j = jnp.maximum(k - s, 0)
        return remote(own(c) if s == 0 else view(j, c), view(j, c), rs.at[s, c], rr.at[s, c], right)

    def to_left(s, c):
        j = jnp.minimum(k + s, n - 1)
        return remote(own(c) if s == 0 else view(j, c), view(j, c), ls.at[s, c], lr.at[s, c], left)

    def across(j, c, mine=False):
        return remote(own(c) if mine else view(j, c), view(j, c), fs.at[j, c], fr.at[j, c], partner)

    for s in range(n - 1):
        for c in range(CHUNKS):
            if s > 0:
                @pl.when(k - s >= 0)
                def _():
                    to_right(s - 1, c).wait_recv()

                @pl.when(k + s < n)
                def _():
                    to_left(s - 1, c).wait_recv()

            @pl.when((k - s >= 0) & (k < n - 1))
            def _():
                to_right(s, c).start()

            @pl.when((k + s < n) & (k > 0))
            def _():
                to_left(s, c).start()

            if s == 0:
                across(k, c, True).start()
            else:
                @pl.when(k - s >= 0)
                def _():
                    across(k - s, c).start()

                @pl.when(k + s < n)
                def _():
                    across(k + s, c).start()
        if s == 0:
            local = pltpu.make_async_copy(own_ref, out_ref.at[k, t], local_sem)
            local.start()
            local.wait()
    s = n - 1
    for c in range(CHUNKS):
        @pl.when(k - s >= 0)
        def _():
            to_right(s - 1, c).wait_recv()
            across(k - s, c).start()

        @pl.when(k + s < n)
        def _():
            to_left(s - 1, c).wait_recv()
            across(k + s, c).start()
    for s in range(n - 1):
        for c in range(CHUNKS):
            @pl.when((k - s >= 0) & (k < n - 1))
            def _():
                to_right(s, c).wait_send()

            @pl.when((k + s < n) & (k > 0))
            def _():
                to_left(s, c).wait_send()
    for j in range(n):
        for c in range(CHUNKS):
            across(j, c).wait_send()
            remote(
                out_ref.at[j, 1 - t, :, pl.ds(c * span, span)],
                out_ref.at[j, 1 - t, :, pl.ds(c * span, span)],
                fs.at[j, c],
                fr.at[j, c],
                partner,
            ).wait_recv()


def gathered(own):
    n = lax.axis_size("kv")
    rows, cols = own.shape
    dma = pltpu.SemaphoreType.DMA
    out = pl.pallas_call(
        functools.partial(gather_kernel, n),
        out_shape=jax.ShapeDtypeStruct((n, 2, rows, cols), own.dtype),
        in_specs=[pl.BlockSpec(memory_space=pltpu.VMEM)],
        out_specs=pl.BlockSpec(memory_space=pltpu.VMEM),
        scratch_shapes=[dma((n - 1, CHUNKS))] * 4 + [dma((n, CHUNKS))] * 2 + [dma],
        compiler_params=pltpu.CompilerParams(
            collective_id=0, has_side_effects=True, vmem_limit_bytes=32 * 1024 * 1024
        ),
        name="gather",
    )(own)
    return out.reshape(n * 2 * rows, cols)


def scatter_kernel(
    n, part, sq, out, sqs, pbuf, rbuf, lbuf, rout, lout, ps, pr, rs, rr, ls, lr, ss, sr
):
    f32 = jnp.float32
    k = lax.axis_index("kv")
    t = lax.axis_index("tp")
    rank = k * 2 + t
    ranks = n * 2
    right = {"kv": lax.rem(k + 1, n)}
    left = {"kv": lax.rem(k + n - 1, n)}
    partner = {"tp": 1 - t}
    span = part.shape[3] // CHUNKS
    barrier = pltpu.get_barrier_semaphore()

    def peer(o):
        p = lax.rem(rank + o, ranks)
        return {"kv": p // 2, "tp": lax.rem(p, 2)}

    for o in range(1, ranks):
        pl.semaphore_signal(barrier, inc=1, device_id=peer(o), device_id_type=MESH)
    pl.semaphore_wait(barrier, ranks - 1)

    def cut(c):
        return pl.ds(c * span, span)

    def across(j, c):
        return remote(
            part.at[j, 1 - t, :, cut(c)], pbuf.at[j, :, cut(c)], ps.at[j, c], pr.at[j, c], partner
        )

    def to_right(d, c):
        return remote(
            rout.at[d, :, cut(c)], rbuf.at[d, :, cut(c)], rs.at[d, c], rr.at[d, c], right
        )

    def to_left(d, c):
        return remote(lout.at[d, :, cut(c)], lbuf.at[d, :, cut(c)], ls.at[d, c], lr.at[d, c], left)

    def square(o):
        p = lax.rem(rank + o, ranks)
        return remote(sq.at[p], sqs.at[rank], ss.at[o], sr.at[o], peer(o))

    order = []
    for i in range(n):
        for j in (n - 1 - i, i):
            if j not in order:
                order.append(j)
    for j in order:
        for c in range(CHUNKS):
            across(j, c).start()
    for o in range(1, ranks):
        square(o).start()
    sqs[rank] = sq[rank]

    def pair(j, c):
        across(j, c).wait_recv()
        return part[j, t, :, cut(c)].astype(f32) + pbuf[j, :, cut(c)].astype(f32)

    for i in range(n - 1):
        for c in range(CHUNKS):
            d = n - 1 - i

            @pl.when((k < d) & (k == 0))
            def _():
                rout[d, :, cut(c)] = pair(d, c).astype(rout.dtype)
                to_right(d, c).start()

            @pl.when((k < d) & (k > 0))
            def _():
                value = pair(d, c)
                to_right(d, c).wait_recv()
                rout[d, :, cut(c)] = (value + rbuf[d, :, cut(c)].astype(f32)).astype(rout.dtype)
                to_right(d, c).start()

            @pl.when((k > i) & (k == n - 1))
            def _():
                lout[i, :, cut(c)] = pair(i, c).astype(lout.dtype)
                to_left(i, c).start()

            @pl.when((k > i) & (k < n - 1))
            def _():
                value = pair(i, c)
                to_left(i, c).wait_recv()
                lout[i, :, cut(c)] = (value + lbuf[i, :, cut(c)].astype(f32)).astype(lout.dtype)
                to_left(i, c).start()

    for c in range(CHUNKS):
        out[:, cut(c)] = pair(k, c)

        @pl.when(k > 0)
        def _():
            to_right(k, c).wait_recv()
            out[:, cut(c)] += rbuf[k, :, cut(c)].astype(f32)

        @pl.when(k < n - 1)
        def _():
            to_left(k, c).wait_recv()
            out[:, cut(c)] += lbuf[k, :, cut(c)].astype(f32)

    for j in range(n):
        for c in range(CHUNKS):
            across(j, c).wait_send()

            @pl.when(k < j)
            def _():
                to_right(j, c).wait_send()

            @pl.when(k > j)
            def _():
                to_left(j, c).wait_send()
    for o in range(1, ranks):
        square(o).wait_send()
        source = lax.rem(rank + ranks - o, ranks)
        remote(sq.at[rank], sqs.at[source], ss.at[o], sr.at[o], peer(o)).wait_recv()


def scattered(partial_value, squares):
    n = lax.axis_size("kv")
    ranks = n * 2
    rows = partial_value.shape[0] // ranks
    cols = partial_value.shape[1]
    squares = jnp.pad(squares.reshape(ranks, 1, rows), ((0, 0), (0, 7), (0, 128 - rows)))
    dma = pltpu.SemaphoreType.DMA
    vmem = pl.BlockSpec(memory_space=pltpu.VMEM)
    kind = partial_value.dtype
    summed, sqs = pl.pallas_call(
        functools.partial(scatter_kernel, n),
        out_shape=[
            jax.ShapeDtypeStruct((rows, cols), jnp.float32),
            jax.ShapeDtypeStruct(squares.shape, jnp.float32),
        ],
        in_specs=[vmem, vmem],
        out_specs=[vmem, vmem],
        scratch_shapes=[pltpu.VMEM((n, rows, cols), kind)] * 5
        + [dma((n, CHUNKS))] * 6
        + [dma((ranks,))] * 2,
        compiler_params=pltpu.CompilerParams(
            collective_id=1, has_side_effects=True, vmem_limit_bytes=32 * 1024 * 1024
        ),
        name="scatter",
    )(partial_value.reshape(n, 2, rows, cols), squares)
    return summed, jnp.sum(sqs[:, 0, :rows], axis=0)


def body(
    tokens,
    norm_gain,
    gate_proj,
    inner_proj,
    write_proj,
    read_proj,
    step_proj,
    step_bias,
    decay_log,
    skip_gain,
    conv_inner,
    conv_write,
    conv_read,
    out_gain,
    out_proj,
    saved_state,
    inner_history,
    write_history,
    read_history,
    last_steps,
    accepted,
):
    device_rank = lax.axis_index(("kv", "tp"))
    seq_count = saved_state.shape[0]
    local_heads = saved_state.shape[1]
    head_dim = saved_state.shape[2]
    proposals = last_steps.shape[1]
    inner_cols = inner_proj.shape[1]
    state_cols = write_proj.shape[1]
    token_count = tokens.shape[0]
    own_rows = tokens.astype(jnp.float32)
    normed_own = (
        own_rows
        * lax.rsqrt(jnp.mean(own_rows * own_rows, axis=-1, keepdims=True) + EPSILON)
        * norm_gain
    ).astype(jnp.bfloat16)
    normed = gathered(normed_own)
    normed = normed.reshape(seq_count, proposals, -1).transpose(1, 0, 2)
    normed = normed.reshape(proposals * seq_count, -1)

    def project(weight):
        out = jnp.dot(normed, weight, preferred_element_type=jnp.float32)
        return out.reshape(proposals, seq_count, -1)

    gate_rows = project(gate_proj).astype(jnp.bfloat16)
    inner_rows = project(inner_proj).astype(jnp.bfloat16)
    write_rows = project(write_proj).astype(jnp.bfloat16)
    read_rows = project(read_proj).astype(jnp.bfloat16)
    first_head = device_rank * local_heads
    steps = lax.dynamic_slice_in_dim(project(step_proj), first_head, local_heads, 2)
    par = lax.dynamic_slice_in_dim(
        jnp.stack([step_bias, decay_log, skip_gain]), first_head, local_heads, 1
    )
    slab = lambda x: x.transpose(1, 0, 2)
    hist_inner, hist_write, hist_read = slab(inner_history), slab(write_history), slab(read_history)
    pieces = (write_rows, read_rows, hist_write, hist_read)
    group_span = lax.axis_size("kv") * lax.axis_size("tp") // GROUPS
    if group_span >= 2:
        pieces = tuple(lax.all_gather(x, "tp", axis=2, tiled=True) for x in pieces)
        kv_rank = lax.axis_index("kv")
        bit_count = (group_span // lax.axis_size("tp")).bit_length() - 1
        for bit in range(bit_count):
            partner = swapped(pieces, "kv", bit)
            lower = jnp.bitwise_and(jnp.right_shift(kv_rank, bit), 1) == 0
            pieces = tuple(
                jnp.where(
                    lower,
                    jnp.concatenate([mine, theirs], axis=2),
                    jnp.concatenate([theirs, mine], axis=2),
                )
                for mine, theirs in zip(pieces, partner)
            )
    write_rows, read_rows, hist_write, hist_read = pieces
    unscaled, squares, base_state = mix(
        device_rank,
        device_rank // group_span,
        accepted[:, None],
        steps,
        slab(last_steps),
        par,
        gate_rows,
        inner_rows,
        write_rows,
        read_rows,
        hist_inner,
        hist_write,
        hist_read,
        conv_inner,
        conv_write,
        conv_read,
        out_gain[None, :],
        saved_state.reshape(seq_count, local_heads * head_dim, -1),
    )
    base_state = base_state.reshape(saved_state.shape)
    unscaled = unscaled.transpose(1, 0, 2).reshape(seq_count * proposals, inner_cols)
    partial_value = jnp.dot(unscaled, out_proj, preferred_element_type=jnp.float32)
    squares = squares[:, :, 0].T.reshape(-1)
    summed, square_own = scattered(partial_value.astype(jnp.bfloat16), squares)
    mixed = (summed * lax.rsqrt(square_own / out_gain.shape[0] + EPSILON)[:, None]).astype(jnp.bfloat16)
    return (mixed, base_state)


def solution(mesh):
    placed = (
        P(("dp", "kv", "tp"), None),
        P(),
        P(None, ("kv", "tp")),
        P(None, ("kv", "tp")),
        P(None, ("kv", "tp")),
        P(None, ("kv", "tp")),
        P(),
        P(),
        P(),
        P(),
        P(),
        P(),
        P(),
        P(),
        P(("kv", "tp"), None),
        P("dp", ("kv", "tp"), None, None),
        P("dp", None, ("kv", "tp")),
        P("dp", None, ("kv", "tp")),
        P("dp", None, ("kv", "tp")),
        P("dp", None, ("kv", "tp")),
        P("dp"),
    )
    return jax.shard_map(
        body,
        mesh=mesh,
        in_specs=placed,
        out_specs=(P(("dp", "kv", "tp"), None), P("dp", ("kv", "tp"), None, None)),
        check_vma=False,
    )
```

```python
import functools

import jax
import jax.numpy as jnp
from jax import lax
from jax.experimental import pallas as pl
from jax.experimental.pallas import tpu as pltpu
from jax.sharding import PartitionSpec as P

GROUPS = 8
EPSILON = 0.1
BLOCK = 8
highest = lax.Precision.HIGHEST


def swapped(value, axis, stride):
    mask = 2**stride
    pairs = [(source, source ^ mask) for source in range(lax.axis_size(axis))]
    return lax.ppermute(value, axis, pairs)


def mix_kernel(
    rank_ref,
    acc_ref,
    steps_ref,
    last_ref,
    par_ref,
    gate_ref,
    inner_ref,
    write_ref,
    read_ref,
    hist_inner_ref,
    hist_write_ref,
    hist_read_ref,
    taps_inner_ref,
    taps_write_ref,
    taps_read_ref,
    gain_ref,
    expand_ref,
    state_ref,
    un_ref,
    sq_ref,
    base_ref,
):
    f32 = jnp.float32
    props = steps_ref.shape[0]
    heads = last_ref.shape[2]
    cols = inner_ref.shape[2]
    states = write_ref.shape[2]
    head_dim = cols // heads
    hist = hist_inner_ref.shape[0]
    width = taps_inner_ref.shape[0]
    acc = acc_ref[...]

    def silu(x):
        return x / (1.0 + jnp.exp(-x))

    def slabs(ref):
        return [ref[k].astype(f32) for k in range(ref.shape[0])]

    round_bf = lambda x: x.astype(jnp.bfloat16).astype(f32)

    def conv(rows, taps_ref):
        taps = taps_ref[...].astype(f32)
        res = []
        for r in range(len(rows) - width + 1):
            v = taps[0:1] * rows[r]
            for k in range(1, width):
                v = v + taps[k : k + 1] * rows[r + k]
            res.append(silu(v))
        return res

    def current(h, new_ref):
        where_at = jnp.broadcast_to(acc, h[0].shape)
        rows = []
        for k in range(width - 1):
            r = h[k]
            for v in range(1, hist - width + 2):
                r = jnp.where(where_at == v, h[k + v], r)
            rows.append(r)
        return rows + [round_bf(x) for x in slabs(new_ref)]

    h_inner = slabs(hist_inner_ref)
    inner_old = conv(h_inner, taps_inner_ref)
    inner_new = conv(current(h_inner, inner_ref), taps_inner_ref)
    h_write = slabs(hist_write_ref)
    write_old = [round_bf(x) for x in conv(h_write, taps_write_ref)]
    write_new = [round_bf(x) for x in conv(current(h_write, write_ref), taps_write_ref)]
    read_new = [round_bf(x) for x in conv(current(slabs(hist_read_ref), read_ref), taps_read_ref)]

    bias = par_ref[0:1]
    rate = -jnp.exp(par_ref[1:2])
    skip = par_ref[2:3]
    acc_h = jnp.broadcast_to(acc, (BLOCK, heads))
    masks = [jnp.where(acc_h > t, 1.0, 0.0) for t in range(props)]
    logs = [rate * last_ref[t] * masks[t] for t in range(props)]
    coefs = [None] * props
    tail = jnp.zeros((BLOCK, heads), f32)
    for t in reversed(range(props)):
        coefs[t] = masks[t] * jnp.exp(tail) * last_ref[t]
        tail = tail + logs[t]
    decay = jnp.exp(tail)
    step = []
    for t in range(props):
        x = steps_ref[t][:, :heads] + bias
        step.append(jnp.maximum(x, 0.0) + jnp.log1p(jnp.exp(-jnp.abs(x))))
    cums = []
    for t in range(props):
        cums.append(rate * step[t] + (cums[-1] if cums else 0.0))
    where_of = {}
    for i in range(props):
        for j in range(i + 1):
            score = jnp.sum(read_new[i] * write_new[j], axis=-1, keepdims=True)
            c = jnp.exp(cums[i] - cums[j]) * step[j] * score
            if i == j:
                c = c + skip
            where_of[(i, j)] = len(coefs)
            coefs.append(c)
    first_cum = len(coefs)
    for i in range(props):
        coefs.append(jnp.exp(cums[i]))
    wide = jnp.dot(
        jnp.concatenate(coefs, axis=0),
        expand_ref[...],
        precision=highest,
        preferred_element_type=f32,
    )

    def at(k):
        return wide[k * BLOCK : (k + 1) * BLOCK]

    left = jnp.concatenate([at(t) * inner_old[t] for t in range(props)], axis=0)
    high = round_bf(left)
    both = jnp.concatenate([high, left - high], axis=0)
    turned = jnp.transpose(both).astype(jnp.bfloat16)
    write_all = jnp.concatenate(write_old + write_old, axis=0)
    read_all = jnp.concatenate(read_new, axis=0)
    seq_w = lax.broadcasted_iota(jnp.int32, write_all.shape, 0) % BLOCK
    seq_r = lax.broadcasted_iota(jnp.int32, read_all.shape, 0) % BLOCK
    carried = jnp.zeros((props * BLOCK, cols), f32)
    for s in range(BLOCK):
        right = jnp.where(seq_w == s, write_all, 0.0).astype(jnp.bfloat16)
        update = jnp.dot(turned, right, preferred_element_type=f32)
        parts = []
        for h in range(heads):
            lo, hi = h * head_dim, (h + 1) * head_dim
            d = jnp.broadcast_to(decay[s : s + 1, h : h + 1], (head_dim, states))
            new = d * state_ref[s, lo:hi, :] + update[lo:hi]
            base_ref[s, lo:hi, :] = new
            parts.append(new.astype(jnp.bfloat16))
        asked = jnp.where(seq_r == s, read_all, 0.0).astype(jnp.bfloat16)
        carried = carried + lax.dot_general(
            asked,
            jnp.concatenate(parts, axis=0),
            (((1,), (1,)), ((), ())),
            preferred_element_type=f32,
        )
    for i in range(props):
        y = at(first_cum + i) * carried[i * BLOCK : (i + 1) * BLOCK]
        for j in range(i + 1):
            y = y + at(where_of[(i, j)]) * inner_new[j]
        g = y * silu(gate_ref[i].astype(f32))
        sq_ref[i] = jnp.broadcast_to(jnp.sum(g * g, axis=-1, keepdims=True), sq_ref.shape[1:])
        un_ref[i] = (g * gain_ref[...]).astype(un_ref.dtype)


def mix(rank, group, acc, last, par, gate, inner, small, hi, hw, hr, ci, cw, cr, gain, state):
    props, seqs, heads = last.shape
    cols, states = state.shape[1], state.shape[2]
    expand = (jnp.arange(cols)[None, :] // (cols // heads) == jnp.arange(heads)[:, None]).astype(
        jnp.float32
    )
    hist = hi.shape[0]
    width = ci.shape[0]

    def slab(lead, last_dim):
        return pl.BlockSpec((lead, BLOCK, last_dim), lambda g, r: (0, g, 0))

    def piece(which):
        return pl.BlockSpec((props, BLOCK, states), lambda g, r: (0, g, which))

    def own(rows, last_dim, which):
        return pl.BlockSpec((rows, last_dim), lambda g, r: (0, r[which]))

    state_spec = pl.BlockSpec((BLOCK, cols, states), lambda g, r: (g, 0, 0))
    return pl.pallas_call(
        mix_kernel,
        grid_spec=pltpu.PrefetchScalarGridSpec(
            num_scalar_prefetch=1,
            grid=(seqs // BLOCK,),
            in_specs=[
                pl.BlockSpec((BLOCK, 1), lambda g, r: (g, 0)),
                piece(2),
                slab(props, heads),
                pl.BlockSpec(par.shape, lambda g, r: (0, 0)),
                slab(props, cols),
                slab(props, cols),
                piece(0),
                piece(1),
                slab(hist, cols),
                slab(hist, states),
                slab(hist, states),
                own(width, cols, 0),
                own(width, states, 1),
                own(width, states, 1),
                own(1, cols, 0),
                pl.BlockSpec(expand.shape, lambda g, r: (0, 0)),
                state_spec,
            ],
            out_specs=[slab(props, cols), slab(props, 128), state_spec],
        ),
        out_shape=[
            jax.ShapeDtypeStruct((props, seqs, cols), jnp.bfloat16),
            jax.ShapeDtypeStruct((props, seqs, 128), jnp.float32),
            jax.ShapeDtypeStruct(state.shape, jnp.float32),
        ],
        compiler_params=pltpu.CompilerParams(
            dimension_semantics=("arbitrary",), vmem_limit_bytes=48 * 1024 * 1024
        ),
        name="mix",
    )(
        jnp.stack([rank, group]).astype(jnp.int32),
        acc, small, last, par, gate, inner, small, small, hi, hw, hr, ci, cw, cr, gain, expand, state,
    )


MESH = pl.DeviceIdType.MESH
CHUNKS = 2


def remote(src, dst, send, recv, where):
    return pltpu.make_async_remote_copy(
        src_ref=src, dst_ref=dst, send_sem=send, recv_sem=recv, device_id=where, device_id_type=MESH
    )


def gather_kernel(n, own_ref, out_ref, rs, rr, ls, lr, fs, fr, local_sem):
    k = lax.axis_index("kv")
    t = lax.axis_index("tp")
    right = {"kv": lax.rem(k + 1, n)}
    left = {"kv": lax.rem(k + n - 1, n)}
    partner = {"tp": 1 - t}
    span = own_ref.shape[1] // CHUNKS
    barrier = pltpu.get_barrier_semaphore()
    pl.semaphore_signal(barrier, inc=1, device_id=partner, device_id_type=MESH)

    @pl.when(k < n - 1)
    def _():
        pl.semaphore_signal(barrier, inc=1, device_id=right, device_id_type=MESH)

    @pl.when(k > 0)
    def _():
        pl.semaphore_signal(barrier, inc=1, device_id=left, device_id_type=MESH)

    inner = (k > 0) & (k < n - 1)

    @pl.when(inner)
    def _():
        pl.semaphore_wait(barrier, 3)

    @pl.when(jnp.logical_not(inner))
    def _():
        pl.semaphore_wait(barrier, 2)

    def view(j, c):
        return out_ref.at[j, t, :, pl.ds(c * span, span)]

    def own(c):
        return own_ref.at[:, pl.ds(c * span, span)]

    def to_right(s, c):
        j = jnp.maximum(k - s, 0)
        return remote(own(c) if s == 0 else view(j, c), view(j, c), rs.at[s, c], rr.at[s, c], right)

    def to_left(s, c):
        j = jnp.minimum(k + s, n - 1)
        return remote(own(c) if s == 0 else view(j, c), view(j, c), ls.at[s, c], lr.at[s, c], left)

    def across(j, c, mine=False):
        return remote(own(c) if mine else view(j, c), view(j, c), fs.at[j, c], fr.at[j, c], partner)

    for s in range(n - 1):
        for c in range(CHUNKS):
            if s > 0:
                @pl.when(k - s >= 0)
                def _():
                    to_right(s - 1, c).wait_recv()

                @pl.when(k + s < n)
                def _():
                    to_left(s - 1, c).wait_recv()

            @pl.when((k - s >= 0) & (k < n - 1))
            def _():
                to_right(s, c).start()

            @pl.when((k + s < n) & (k > 0))
            def _():
                to_left(s, c).start()

            if s == 0:
                across(k, c, True).start()
            else:
                @pl.when(k - s >= 0)
                def _():
                    across(k - s, c).start()

                @pl.when(k + s < n)
                def _():
                    across(k + s, c).start()
        if s == 0:
            local = pltpu.make_async_copy(own_ref, out_ref.at[k, t], local_sem)
            local.start()
            local.wait()
    s = n - 1
    for c in range(CHUNKS):
        @pl.when(k - s >= 0)
        def _():
            to_right(s - 1, c).wait_recv()
            across(k - s, c).start()

        @pl.when(k + s < n)
        def _():
            to_left(s - 1, c).wait_recv()
            across(k + s, c).start()
    for s in range(n - 1):
        for c in range(CHUNKS):
            @pl.when((k - s >= 0) & (k < n - 1))
            def _():
                to_right(s, c).wait_send()

            @pl.when((k + s < n) & (k > 0))
            def _():
                to_left(s, c).wait_send()
    for j in range(n):
        for c in range(CHUNKS):
            across(j, c).wait_send()
            remote(
                out_ref.at[j, 1 - t, :, pl.ds(c * span, span)],
                out_ref.at[j, 1 - t, :, pl.ds(c * span, span)],
                fs.at[j, c],
                fr.at[j, c],
                partner,
            ).wait_recv()


def gathered(own):
    n = lax.axis_size("kv")
    rows, cols = own.shape
    dma = pltpu.SemaphoreType.DMA
    out = pl.pallas_call(
        functools.partial(gather_kernel, n),
        out_shape=jax.ShapeDtypeStruct((n, 2, rows, cols), own.dtype),
        in_specs=[pl.BlockSpec(memory_space=pltpu.VMEM)],
        out_specs=pl.BlockSpec(memory_space=pltpu.VMEM),
        scratch_shapes=[dma((n - 1, CHUNKS))] * 4 + [dma((n, CHUNKS))] * 2 + [dma],
        compiler_params=pltpu.CompilerParams(
            collective_id=0, has_side_effects=True, vmem_limit_bytes=32 * 1024 * 1024
        ),
        name="gather",
    )(own)
    return out.reshape(n * 2 * rows, cols)


def scatter_kernel(
    n, part, sq, out, sqs, pbuf, rbuf, lbuf, rout, lout, ps, pr, rs, rr, ls, lr, ss, sr
):
    f32 = jnp.float32
    k = lax.axis_index("kv")
    t = lax.axis_index("tp")
    rank = k * 2 + t
    ranks = n * 2
    right = {"kv": lax.rem(k + 1, n)}
    left = {"kv": lax.rem(k + n - 1, n)}
    partner = {"tp": 1 - t}
    span = part.shape[3] // CHUNKS
    barrier = pltpu.get_barrier_semaphore()

    def peer(o):
        p = lax.rem(rank + o, ranks)
        return {"kv": p // 2, "tp": lax.rem(p, 2)}

    for o in range(1, ranks):
        pl.semaphore_signal(barrier, inc=1, device_id=peer(o), device_id_type=MESH)
    pl.semaphore_wait(barrier, ranks - 1)

    def cut(c):
        return pl.ds(c * span, span)

    def across(j, c):
        return remote(
            part.at[j, 1 - t, :, cut(c)], pbuf.at[j, :, cut(c)], ps.at[j, c], pr.at[j, c], partner
        )

    def to_right(d, c):
        return remote(
            rout.at[d, :, cut(c)], rbuf.at[d, :, cut(c)], rs.at[d, c], rr.at[d, c], right
        )

    def to_left(d, c):
        return remote(lout.at[d, :, cut(c)], lbuf.at[d, :, cut(c)], ls.at[d, c], lr.at[d, c], left)

    def square(o):
        p = lax.rem(rank + o, ranks)
        return remote(sq.at[p], sqs.at[rank], ss.at[o], sr.at[o], peer(o))

    low = k < n // 2
    for i in range(n):
        j = jnp.where(low, n - 1 - i, i)
        for c in range(CHUNKS):
            across(j, c).start()
    for o in range(1, ranks):
        square(o).start()
    sqs[rank] = sq[rank]

    def pair(j, c):
        across(j, c).wait_recv()
        return part[j, t, :, cut(c)].astype(f32) + pbuf[j, :, cut(c)].astype(f32)

    def rightward():
        for d in range(n - 1, 0, -1):
            for c in range(CHUNKS):
                @pl.when((k < d) & (k == 0))
                def _():
                    rout[d, :, cut(c)] = pair(d, c).astype(rout.dtype)
                    to_right(d, c).start()

                @pl.when((k < d) & (k > 0))
                def _():
                    value = pair(d, c)
                    to_right(d, c).wait_recv()
                    rout[d, :, cut(c)] = (value + rbuf[d, :, cut(c)].astype(f32)).astype(rout.dtype)
                    to_right(d, c).start()

    def leftward():
        for d in range(n - 1):
            for c in range(CHUNKS):
                @pl.when((k > d) & (k == n - 1))
                def _():
                    lout[d, :, cut(c)] = pair(d, c).astype(lout.dtype)
                    to_left(d, c).start()

                @pl.when((k > d) & (k < n - 1))
                def _():
                    value = pair(d, c)
                    to_left(d, c).wait_recv()
                    lout[d, :, cut(c)] = (value + lbuf[d, :, cut(c)].astype(f32)).astype(lout.dtype)
                    to_left(d, c).start()

    @pl.when(k < n // 2)
    def _():
        rightward()
        leftward()

    @pl.when(k >= n // 2)
    def _():
        leftward()
        rightward()

    for c in range(CHUNKS):
        out[:, cut(c)] = pair(k, c)

        @pl.when(k > 0)
        def _():
            to_right(k, c).wait_recv()
            out[:, cut(c)] += rbuf[k, :, cut(c)].astype(f32)

        @pl.when(k < n - 1)
        def _():
            to_left(k, c).wait_recv()
            out[:, cut(c)] += lbuf[k, :, cut(c)].astype(f32)

    for j in range(n):
        for c in range(CHUNKS):
            across(j, c).wait_send()

            @pl.when(k < j)
            def _():
                to_right(j, c).wait_send()

            @pl.when(k > j)
            def _():
                to_left(j, c).wait_send()
    for o in range(1, ranks):
        square(o).wait_send()
        source = lax.rem(rank + ranks - o, ranks)
        remote(sq.at[rank], sqs.at[source], ss.at[o], sr.at[o], peer(o)).wait_recv()


def scattered(partial_value, squares):
    n = lax.axis_size("kv")
    ranks = n * 2
    rows = partial_value.shape[0] // ranks
    cols = partial_value.shape[1]
    squares = jnp.pad(squares.reshape(ranks, 1, rows), ((0, 0), (0, 7), (0, 128 - rows)))
    dma = pltpu.SemaphoreType.DMA
    vmem = pl.BlockSpec(memory_space=pltpu.VMEM)
    kind = partial_value.dtype
    summed, sqs = pl.pallas_call(
        functools.partial(scatter_kernel, n),
        out_shape=[
            jax.ShapeDtypeStruct((rows, cols), jnp.float32),
            jax.ShapeDtypeStruct(squares.shape, jnp.float32),
        ],
        in_specs=[vmem, vmem],
        out_specs=[vmem, vmem],
        scratch_shapes=[pltpu.VMEM((n, rows, cols), kind)] * 5
        + [dma((n, CHUNKS))] * 6
        + [dma((ranks,))] * 2,
        compiler_params=pltpu.CompilerParams(
            collective_id=1, has_side_effects=True, vmem_limit_bytes=32 * 1024 * 1024
        ),
        name="scatter",
    )(partial_value.reshape(n, 2, rows, cols), squares)
    return summed, jnp.sum(sqs[:, 0, :rows], axis=0)


def body(
    tokens,
    norm_gain,
    gate_proj,
    inner_proj,
    write_proj,
    read_proj,
    step_proj,
    step_bias,
    decay_log,
    skip_gain,
    conv_inner,
    conv_write,
    conv_read,
    out_gain,
    out_proj,
    saved_state,
    inner_history,
    write_history,
    read_history,
    last_steps,
    accepted,
):
    device_rank = lax.axis_index(("kv", "tp"))
    seq_count = saved_state.shape[0]
    local_heads = saved_state.shape[1]
    head_dim = saved_state.shape[2]
    proposals = last_steps.shape[1]
    inner_cols = inner_proj.shape[1]
    state_cols = write_proj.shape[1]
    token_count = tokens.shape[0]
    own_rows = tokens.astype(jnp.float32)
    normed_own = (
        own_rows
        * lax.rsqrt(jnp.mean(own_rows * own_rows, axis=-1, keepdims=True) + EPSILON)
        * norm_gain
    ).astype(jnp.bfloat16)
    normed = gathered(normed_own)
    normed = normed.reshape(seq_count, proposals, -1).transpose(1, 0, 2)
    normed = normed.reshape(proposals * seq_count, -1)

    def project(weight):
        out = jnp.dot(normed, weight, preferred_element_type=jnp.float32)
        return out.reshape(proposals, seq_count, -1)

    gate_rows = project(gate_proj).astype(jnp.bfloat16)
    inner_rows = project(inner_proj).astype(jnp.bfloat16)
    first_head = device_rank * local_heads
    state_cols = write_proj.shape[1]
    states = saved_state.shape[3]
    step_local = lax.dynamic_slice_in_dim(step_proj, first_head, local_heads, 1)
    step_local = jnp.pad(step_local, ((0, 0), (0, states - local_heads)))
    small = project(jnp.concatenate([write_proj, read_proj, step_local], axis=1))
    par = lax.dynamic_slice_in_dim(
        jnp.stack([step_bias, decay_log, skip_gain]), first_head, local_heads, 1
    )
    slab = lambda x: x.transpose(1, 0, 2)
    hist_inner, hist_write, hist_read = slab(inner_history), slab(write_history), slab(read_history)
    group_span = lax.axis_size("kv") * lax.axis_size("tp") // GROUPS
    if group_span >= 2:
        write_rows = small[:, :, :state_cols].astype(jnp.bfloat16)
        read_rows = small[:, :, state_cols : 2 * state_cols].astype(jnp.bfloat16)
        pieces = (write_rows, read_rows, hist_write, hist_read)
        pieces = tuple(lax.all_gather(x, "tp", axis=2, tiled=True) for x in pieces)
        kv_rank = lax.axis_index("kv")
        bit_count = (group_span // lax.axis_size("tp")).bit_length() - 1
        for bit in range(bit_count):
            partner = swapped(pieces, "kv", bit)
            lower = jnp.bitwise_and(jnp.right_shift(kv_rank, bit), 1) == 0
            pieces = tuple(
                jnp.where(
                    lower,
                    jnp.concatenate([mine, theirs], axis=2),
                    jnp.concatenate([theirs, mine], axis=2),
                )
                for mine, theirs in zip(pieces, partner)
            )
        write_rows, read_rows, hist_write, hist_read = pieces
        small = jnp.concatenate(
            [
                write_rows.astype(jnp.float32),
                read_rows.astype(jnp.float32),
                small[:, :, 2 * state_cols :],
            ],
            axis=2,
        )
    unscaled, squares, base_state = mix(
        device_rank,
        device_rank // group_span,
        accepted[:, None],
        slab(last_steps),
        par,
        gate_rows,
        inner_rows,
        small,
        hist_inner,
        hist_write,
        hist_read,
        conv_inner,
        conv_write,
        conv_read,
        out_gain[None, :],
        saved_state.reshape(seq_count, local_heads * head_dim, -1),
    )
    base_state = base_state.reshape(saved_state.shape)
    unscaled = unscaled.transpose(1, 0, 2).reshape(seq_count * proposals, inner_cols)
    partial_value = jnp.dot(unscaled, out_proj, preferred_element_type=jnp.float32)
    squares = squares[:, :, 0].T.reshape(-1)
    summed, square_own = scattered(partial_value.astype(jnp.bfloat16), squares)
    mixed = (summed * lax.rsqrt(square_own / out_gain.shape[0] + EPSILON)[:, None]).astype(jnp.bfloat16)
    return (mixed, base_state)


def solution(mesh):
    placed = (
        P(("dp", "kv", "tp"), None),
        P(),
        P(None, ("kv", "tp")),
        P(None, ("kv", "tp")),
        P(None, ("kv", "tp")),
        P(None, ("kv", "tp")),
        P(),
        P(),
        P(),
        P(),
        P(),
        P(),
        P(),
        P(),
        P(("kv", "tp"), None),
        P("dp", ("kv", "tp"), None, None),
        P("dp", None, ("kv", "tp")),
        P("dp", None, ("kv", "tp")),
        P("dp", None, ("kv", "tp")),
        P("dp", None, ("kv", "tp")),
        P("dp"),
    )
    return jax.shard_map(
        body,
        mesh=mesh,
        in_specs=placed,
        out_specs=(P(("dp", "kv", "tp"), None), P("dp", ("kv", "tp"), None, None)),
        check_vma=False,
    )
```

```python
import functools

import jax
import jax.numpy as jnp
from jax import lax
from jax.experimental import pallas as pl
from jax.experimental.pallas import tpu as pltpu
from jax.sharding import PartitionSpec as P

GROUPS = 8
EPSILON = 0.1
BLOCK = 8
highest = lax.Precision.HIGHEST


def swapped(value, axis, stride):
    mask = 2**stride
    pairs = [(source, source ^ mask) for source in range(lax.axis_size(axis))]
    return lax.ppermute(value, axis, pairs)


def mix_kernel(
    rank_ref,
    acc_ref,
    steps_ref,
    last_ref,
    par_ref,
    gate_ref,
    inner_ref,
    write_ref,
    read_ref,
    hist_inner_ref,
    hist_write_ref,
    hist_read_ref,
    taps_inner_ref,
    taps_write_ref,
    taps_read_ref,
    gain_ref,
    expand_ref,
    state_ref,
    un_ref,
    sq_ref,
    base_ref,
):
    f32 = jnp.float32
    props = steps_ref.shape[0]
    heads = last_ref.shape[2]
    cols = inner_ref.shape[2]
    states = write_ref.shape[2]
    head_dim = cols // heads
    hist = hist_inner_ref.shape[0]
    width = taps_inner_ref.shape[0]
    acc = acc_ref[...]

    def silu(x):
        return x / (1.0 + jnp.exp(-x))

    def slabs(ref):
        return [ref[k].astype(f32) for k in range(ref.shape[0])]

    round_bf = lambda x: x.astype(jnp.bfloat16).astype(f32)

    def conv(rows, taps_ref):
        taps = taps_ref[...].astype(f32)
        res = []
        for r in range(len(rows) - width + 1):
            v = taps[0:1] * rows[r]
            for k in range(1, width):
                v = v + taps[k : k + 1] * rows[r + k]
            res.append(silu(v))
        return res

    def current(h, new_ref):
        where_at = jnp.broadcast_to(acc, h[0].shape)
        rows = []
        for k in range(width - 1):
            r = h[k]
            for v in range(1, hist - width + 2):
                r = jnp.where(where_at == v, h[k + v], r)
            rows.append(r)
        return rows + [round_bf(x) for x in slabs(new_ref)]

    h_inner = slabs(hist_inner_ref)
    inner_old = conv(h_inner, taps_inner_ref)
    inner_new = conv(current(h_inner, inner_ref), taps_inner_ref)
    h_write = slabs(hist_write_ref)
    write_old = [round_bf(x) for x in conv(h_write, taps_write_ref)]
    write_new = [round_bf(x) for x in conv(current(h_write, write_ref), taps_write_ref)]
    read_new = [round_bf(x) for x in conv(current(slabs(hist_read_ref), read_ref), taps_read_ref)]

    bias = par_ref[0:1]
    rate = -jnp.exp(par_ref[1:2])
    skip = par_ref[2:3]
    acc_h = jnp.broadcast_to(acc, (BLOCK, heads))
    masks = [jnp.where(acc_h > t, 1.0, 0.0) for t in range(props)]
    logs = [rate * last_ref[t] * masks[t] for t in range(props)]
    coefs = [None] * props
    tail = jnp.zeros((BLOCK, heads), f32)
    for t in reversed(range(props)):
        coefs[t] = masks[t] * jnp.exp(tail) * last_ref[t]
        tail = tail + logs[t]
    decay = jnp.exp(tail)
    step = []
    for t in range(props):
        x = steps_ref[t][:, :heads] + bias
        step.append(jnp.maximum(x, 0.0) + jnp.log1p(jnp.exp(-jnp.abs(x))))
    cums = []
    for t in range(props):
        cums.append(rate * step[t] + (cums[-1] if cums else 0.0))
    where_of = {}
    for i in range(props):
        for j in range(i + 1):
            score = jnp.sum(read_new[i] * write_new[j], axis=-1, keepdims=True)
            c = jnp.exp(cums[i] - cums[j]) * step[j] * score
            if i == j:
                c = c + skip
            where_of[(i, j)] = len(coefs)
            coefs.append(c)
    first_cum = len(coefs)
    for i in range(props):
        coefs.append(jnp.exp(cums[i]))
    wide = jnp.dot(
        jnp.concatenate(coefs, axis=0),
        expand_ref[...],
        precision=highest,
        preferred_element_type=f32,
    )

    def at(k):
        return wide[k * BLOCK : (k + 1) * BLOCK]

    left = jnp.concatenate([at(t) * inner_old[t] for t in range(props)], axis=0)
    high = round_bf(left)
    both = jnp.concatenate([high, left - high], axis=0)
    turned = jnp.transpose(both).astype(jnp.bfloat16)
    write_all = jnp.concatenate(write_old + write_old, axis=0)
    read_all = jnp.concatenate(read_new, axis=0)
    seq_w = lax.broadcasted_iota(jnp.int32, write_all.shape, 0) % BLOCK
    seq_r = lax.broadcasted_iota(jnp.int32, read_all.shape, 0) % BLOCK
    carried = jnp.zeros((props * BLOCK, cols), f32)
    for s in range(BLOCK):
        right = jnp.where(seq_w == s, write_all, 0.0).astype(jnp.bfloat16)
        update = jnp.dot(turned, right, preferred_element_type=f32)
        parts = []
        for h in range(heads):
            lo, hi = h * head_dim, (h + 1) * head_dim
            d = jnp.broadcast_to(decay[s : s + 1, h : h + 1], (head_dim, states))
            new = d * state_ref[s, lo:hi, :] + update[lo:hi]
            base_ref[s, lo:hi, :] = new
            parts.append(new.astype(jnp.bfloat16))
        asked = jnp.where(seq_r == s, read_all, 0.0).astype(jnp.bfloat16)
        carried = carried + lax.dot_general(
            asked,
            jnp.concatenate(parts, axis=0),
            (((1,), (1,)), ((), ())),
            preferred_element_type=f32,
        )
    for i in range(props):
        y = at(first_cum + i) * carried[i * BLOCK : (i + 1) * BLOCK]
        for j in range(i + 1):
            y = y + at(where_of[(i, j)]) * inner_new[j]
        g = y * silu(gate_ref[i].astype(f32))
        sq_ref[i] = jnp.broadcast_to(jnp.sum(g * g, axis=-1, keepdims=True), sq_ref.shape[1:])
        un_ref[i] = (g * gain_ref[...]).astype(un_ref.dtype)


def mix(rank, group, acc, last, par, gate, inner, small, hi, hw, hr, ci, cw, cr, gain, state):
    props, seqs, heads = last.shape
    cols, states = state.shape[1], state.shape[2]
    expand = (jnp.arange(cols)[None, :] // (cols // heads) == jnp.arange(heads)[:, None]).astype(
        jnp.float32
    )
    hist = hi.shape[0]
    width = ci.shape[0]

    def slab(lead, last_dim):
        return pl.BlockSpec((lead, BLOCK, last_dim), lambda g, r: (0, g, 0))

    def piece(which):
        return pl.BlockSpec((props, BLOCK, states), lambda g, r: (0, g, which))

    def own(rows, last_dim, which):
        return pl.BlockSpec((rows, last_dim), lambda g, r: (0, r[which]))

    state_spec = pl.BlockSpec((BLOCK, cols, states), lambda g, r: (g, 0, 0))
    return pl.pallas_call(
        mix_kernel,
        grid_spec=pltpu.PrefetchScalarGridSpec(
            num_scalar_prefetch=1,
            grid=(seqs // BLOCK,),
            in_specs=[
                pl.BlockSpec((BLOCK, 1), lambda g, r: (g, 0)),
                piece(2),
                slab(props, heads),
                pl.BlockSpec(par.shape, lambda g, r: (0, 0)),
                slab(props, cols),
                slab(props, cols),
                piece(0),
                piece(1),
                slab(hist, cols),
                slab(hist, states),
                slab(hist, states),
                own(width, cols, 0),
                own(width, states, 1),
                own(width, states, 1),
                own(1, cols, 0),
                pl.BlockSpec(expand.shape, lambda g, r: (0, 0)),
                state_spec,
            ],
            out_specs=[slab(props, cols), slab(props, 128), state_spec],
        ),
        out_shape=[
            jax.ShapeDtypeStruct((props, seqs, cols), jnp.bfloat16),
            jax.ShapeDtypeStruct((props, seqs, 128), jnp.float32),
            jax.ShapeDtypeStruct(state.shape, jnp.float32),
        ],
        compiler_params=pltpu.CompilerParams(
            dimension_semantics=("arbitrary",), vmem_limit_bytes=48 * 1024 * 1024
        ),
        name="mix",
    )(
        jnp.stack([rank, group]).astype(jnp.int32),
        acc, small, last, par, gate, inner, small, small, hi, hw, hr, ci, cw, cr, gain, expand, state,
    )


MESH = pl.DeviceIdType.MESH
CHUNKS = 4


def remote(src, dst, send, recv, where):
    return pltpu.make_async_remote_copy(
        src_ref=src, dst_ref=dst, send_sem=send, recv_sem=recv, device_id=where, device_id_type=MESH
    )


def gather_kernel(n, own_ref, out_ref, rs, rr, ls, lr, fs, fr, local_sem):
    k = lax.axis_index("kv")
    t = lax.axis_index("tp")
    right = {"kv": lax.rem(k + 1, n)}
    left = {"kv": lax.rem(k + n - 1, n)}
    partner = {"tp": 1 - t}
    span = own_ref.shape[1] // CHUNKS
    barrier = pltpu.get_barrier_semaphore()
    pl.semaphore_signal(barrier, inc=1, device_id=partner, device_id_type=MESH)

    @pl.when(k < n - 1)
    def _():
        pl.semaphore_signal(barrier, inc=1, device_id=right, device_id_type=MESH)

    @pl.when(k > 0)
    def _():
        pl.semaphore_signal(barrier, inc=1, device_id=left, device_id_type=MESH)

    inner = (k > 0) & (k < n - 1)

    @pl.when(inner)
    def _():
        pl.semaphore_wait(barrier, 3)

    @pl.when(jnp.logical_not(inner))
    def _():
        pl.semaphore_wait(barrier, 2)

    def view(j, c):
        return out_ref.at[j, t, :, pl.ds(c * span, span)]

    def own(c):
        return own_ref.at[:, pl.ds(c * span, span)]

    def to_right(s, c):
        j = jnp.maximum(k - s, 0)
        return remote(own(c) if s == 0 else view(j, c), view(j, c), rs.at[s, c], rr.at[s, c], right)

    def to_left(s, c):
        j = jnp.minimum(k + s, n - 1)
        return remote(own(c) if s == 0 else view(j, c), view(j, c), ls.at[s, c], lr.at[s, c], left)

    def across(j, c, mine=False):
        return remote(own(c) if mine else view(j, c), view(j, c), fs.at[j, c], fr.at[j, c], partner)

    for s in range(n - 1):
        for c in range(CHUNKS):
            if s > 0:
                @pl.when(k - s >= 0)
                def _():
                    to_right(s - 1, c).wait_recv()

                @pl.when(k + s < n)
                def _():
                    to_left(s - 1, c).wait_recv()

            @pl.when((k - s >= 0) & (k < n - 1))
            def _():
                to_right(s, c).start()

            @pl.when((k + s < n) & (k > 0))
            def _():
                to_left(s, c).start()

            if s == 0:
                across(k, c, True).start()
            else:
                @pl.when(k - s >= 0)
                def _():
                    across(k - s, c).start()

                @pl.when(k + s < n)
                def _():
                    across(k + s, c).start()
        if s == 0:
            local = pltpu.make_async_copy(own_ref, out_ref.at[k, t], local_sem)
            local.start()
            local.wait()
    s = n - 1
    for c in range(CHUNKS):
        @pl.when(k - s >= 0)
        def _():
            to_right(s - 1, c).wait_recv()
            across(k - s, c).start()

        @pl.when(k + s < n)
        def _():
            to_left(s - 1, c).wait_recv()
            across(k + s, c).start()
    for s in range(n - 1):
        for c in range(CHUNKS):
            @pl.when((k - s >= 0) & (k < n - 1))
            def _():
                to_right(s, c).wait_send()

            @pl.when((k + s < n) & (k > 0))
            def _():
                to_left(s, c).wait_send()
    for j in range(n):
        for c in range(CHUNKS):
            across(j, c).wait_send()
            remote(
                out_ref.at[j, 1 - t, :, pl.ds(c * span, span)],
                out_ref.at[j, 1 - t, :, pl.ds(c * span, span)],
                fs.at[j, c],
                fr.at[j, c],
                partner,
            ).wait_recv()


def gathered(own):
    n = lax.axis_size("kv")
    rows, cols = own.shape
    dma = pltpu.SemaphoreType.DMA
    out = pl.pallas_call(
        functools.partial(gather_kernel, n),
        out_shape=jax.ShapeDtypeStruct((n, 2, rows, cols), own.dtype),
        in_specs=[pl.BlockSpec(memory_space=pltpu.VMEM)],
        out_specs=pl.BlockSpec(memory_space=pltpu.VMEM),
        scratch_shapes=[dma((n - 1, CHUNKS))] * 4 + [dma((n, CHUNKS))] * 2 + [dma],
        compiler_params=pltpu.CompilerParams(
            collective_id=0, has_side_effects=True, vmem_limit_bytes=32 * 1024 * 1024
        ),
        name="gather",
    )(own)
    return out.reshape(n * 2 * rows, cols)


def scatter_kernel(
    n, part, sq, out, sqs, pbuf, rbuf, lbuf, rout, lout, ps, pr, rs, rr, ls, lr, ss, sr
):
    f32 = jnp.float32
    k = lax.axis_index("kv")
    t = lax.axis_index("tp")
    rank = k * 2 + t
    ranks = n * 2
    right = {"kv": lax.rem(k + 1, n)}
    left = {"kv": lax.rem(k + n - 1, n)}
    partner = {"tp": 1 - t}
    span = part.shape[3] // CHUNKS
    barrier = pltpu.get_barrier_semaphore()

    def peer(o):
        p = lax.rem(rank + o, ranks)
        return {"kv": p // 2, "tp": lax.rem(p, 2)}

    for o in range(1, ranks):
        pl.semaphore_signal(barrier, inc=1, device_id=peer(o), device_id_type=MESH)
    pl.semaphore_wait(barrier, ranks - 1)

    def cut(c):
        return pl.ds(c * span, span)

    def across(j, c):
        return remote(
            part.at[j, 1 - t, :, cut(c)], pbuf.at[j, :, cut(c)], ps.at[j, c], pr.at[j, c], partner
        )

    def to_right(d, c):
        return remote(
            rout.at[d, :, cut(c)], rbuf.at[d, :, cut(c)], rs.at[d, c], rr.at[d, c], right
        )

    def to_left(d, c):
        return remote(lout.at[d, :, cut(c)], lbuf.at[d, :, cut(c)], ls.at[d, c], lr.at[d, c], left)

    def square(o):
        p = lax.rem(rank + o, ranks)
        return remote(sq.at[p], sqs.at[rank], ss.at[o], sr.at[o], peer(o))

    low = k < n // 2
    for i in range(n):
        j = jnp.where(low, n - 1 - i, i)
        for c in range(CHUNKS):
            across(j, c).start()
    for o in range(1, ranks):
        square(o).start()
    sqs[rank] = sq[rank]

    def pair(j, c):
        across(j, c).wait_recv()
        return part[j, t, :, cut(c)].astype(f32) + pbuf[j, :, cut(c)].astype(f32)

    def rightward():
        for d in range(n - 1, 0, -1):
            for c in range(CHUNKS):
                @pl.when((k < d) & (k == 0))
                def _():
                    rout[d, :, cut(c)] = pair(d, c).astype(rout.dtype)
                    to_right(d, c).start()

                @pl.when((k < d) & (k > 0))
                def _():
                    value = pair(d, c)
                    to_right(d, c).wait_recv()
                    rout[d, :, cut(c)] = (value + rbuf[d, :, cut(c)].astype(f32)).astype(rout.dtype)
                    to_right(d, c).start()

    def leftward():
        for d in range(n - 1):
            for c in range(CHUNKS):
                @pl.when((k > d) & (k == n - 1))
                def _():
                    lout[d, :, cut(c)] = pair(d, c).astype(lout.dtype)
                    to_left(d, c).start()

                @pl.when((k > d) & (k < n - 1))
                def _():
                    value = pair(d, c)
                    to_left(d, c).wait_recv()
                    lout[d, :, cut(c)] = (value + lbuf[d, :, cut(c)].astype(f32)).astype(lout.dtype)
                    to_left(d, c).start()

    @pl.when(k < n // 2)
    def _():
        rightward()
        leftward()

    @pl.when(k >= n // 2)
    def _():
        leftward()
        rightward()

    for c in range(CHUNKS):
        out[:, cut(c)] = pair(k, c)

        @pl.when(k > 0)
        def _():
            to_right(k, c).wait_recv()
            out[:, cut(c)] += rbuf[k, :, cut(c)].astype(f32)

        @pl.when(k < n - 1)
        def _():
            to_left(k, c).wait_recv()
            out[:, cut(c)] += lbuf[k, :, cut(c)].astype(f32)

    for j in range(n):
        for c in range(CHUNKS):
            across(j, c).wait_send()

            @pl.when(k < j)
            def _():
                to_right(j, c).wait_send()

            @pl.when(k > j)
            def _():
                to_left(j, c).wait_send()
    for o in range(1, ranks):
        square(o).wait_send()
        source = lax.rem(rank + ranks - o, ranks)
        remote(sq.at[rank], sqs.at[source], ss.at[o], sr.at[o], peer(o)).wait_recv()


def scattered(partial_value, squares):
    n = lax.axis_size("kv")
    ranks = n * 2
    rows = partial_value.shape[0] // ranks
    cols = partial_value.shape[1]
    squares = jnp.pad(squares.reshape(ranks, 1, rows), ((0, 0), (0, 7), (0, 128 - rows)))
    dma = pltpu.SemaphoreType.DMA
    vmem = pl.BlockSpec(memory_space=pltpu.VMEM)
    kind = partial_value.dtype
    summed, sqs = pl.pallas_call(
        functools.partial(scatter_kernel, n),
        out_shape=[
            jax.ShapeDtypeStruct((rows, cols), jnp.float32),
            jax.ShapeDtypeStruct(squares.shape, jnp.float32),
        ],
        in_specs=[vmem, vmem],
        out_specs=[vmem, vmem],
        scratch_shapes=[pltpu.VMEM((n, rows, cols), kind)] * 5
        + [dma((n, CHUNKS))] * 6
        + [dma((ranks,))] * 2,
        compiler_params=pltpu.CompilerParams(
            collective_id=1, has_side_effects=True, vmem_limit_bytes=32 * 1024 * 1024
        ),
        name="scatter",
    )(partial_value.reshape(n, 2, rows, cols), squares)
    return summed, jnp.sum(sqs[:, 0, :rows], axis=0)


def body(
    tokens,
    norm_gain,
    gate_proj,
    inner_proj,
    write_proj,
    read_proj,
    step_proj,
    step_bias,
    decay_log,
    skip_gain,
    conv_inner,
    conv_write,
    conv_read,
    out_gain,
    out_proj,
    saved_state,
    inner_history,
    write_history,
    read_history,
    last_steps,
    accepted,
):
    device_rank = lax.axis_index(("kv", "tp"))
    seq_count = saved_state.shape[0]
    local_heads = saved_state.shape[1]
    head_dim = saved_state.shape[2]
    proposals = last_steps.shape[1]
    inner_cols = inner_proj.shape[1]
    state_cols = write_proj.shape[1]
    token_count = tokens.shape[0]
    own_rows = tokens.astype(jnp.float32)
    normed_own = (
        own_rows
        * lax.rsqrt(jnp.mean(own_rows * own_rows, axis=-1, keepdims=True) + EPSILON)
        * norm_gain
    ).astype(jnp.bfloat16)
    normed = gathered(normed_own)
    normed = normed.reshape(seq_count, proposals, -1).transpose(1, 0, 2)
    normed = normed.reshape(proposals * seq_count, -1)

    def project(weight):
        out = jnp.dot(normed, weight, preferred_element_type=jnp.float32)
        return out.reshape(proposals, seq_count, -1)

    gate_rows = project(gate_proj).astype(jnp.bfloat16)
    inner_rows = project(inner_proj).astype(jnp.bfloat16)
    first_head = device_rank * local_heads
    state_cols = write_proj.shape[1]
    states = saved_state.shape[3]
    step_local = lax.dynamic_slice_in_dim(step_proj, first_head, local_heads, 1)
    step_local = jnp.pad(step_local, ((0, 0), (0, states - local_heads)))
    small = project(jnp.concatenate([write_proj, read_proj, step_local], axis=1))
    par = lax.dynamic_slice_in_dim(
        jnp.stack([step_bias, decay_log, skip_gain]), first_head, local_heads, 1
    )
    slab = lambda x: x.transpose(1, 0, 2)
    hist_inner, hist_write, hist_read = slab(inner_history), slab(write_history), slab(read_history)
    group_span = lax.axis_size("kv") * lax.axis_size("tp") // GROUPS
    if group_span >= 2:
        write_rows = small[:, :, :state_cols].astype(jnp.bfloat16)
        read_rows = small[:, :, state_cols : 2 * state_cols].astype(jnp.bfloat16)
        pieces = (write_rows, read_rows, hist_write, hist_read)
        pieces = tuple(lax.all_gather(x, "tp", axis=2, tiled=True) for x in pieces)
        kv_rank = lax.axis_index("kv")
        bit_count = (group_span // lax.axis_size("tp")).bit_length() - 1
        for bit in range(bit_count):
            partner = swapped(pieces, "kv", bit)
            lower = jnp.bitwise_and(jnp.right_shift(kv_rank, bit), 1) == 0
            pieces = tuple(
                jnp.where(
                    lower,
                    jnp.concatenate([mine, theirs], axis=2),
                    jnp.concatenate([theirs, mine], axis=2),
                )
                for mine, theirs in zip(pieces, partner)
            )
        write_rows, read_rows, hist_write, hist_read = pieces
        small = jnp.concatenate(
            [
                write_rows.astype(jnp.float32),
                read_rows.astype(jnp.float32),
                small[:, :, 2 * state_cols :],
            ],
            axis=2,
        )
    unscaled, squares, base_state = mix(
        device_rank,
        device_rank // group_span,
        accepted[:, None],
        slab(last_steps),
        par,
        gate_rows,
        inner_rows,
        small,
        hist_inner,
        hist_write,
        hist_read,
        conv_inner,
        conv_write,
        conv_read,
        out_gain[None, :],
        saved_state.reshape(seq_count, local_heads * head_dim, -1),
    )
    base_state = base_state.reshape(saved_state.shape)
    unscaled = unscaled.transpose(1, 0, 2).reshape(seq_count * proposals, inner_cols)
    partial_value = jnp.dot(unscaled, out_proj, preferred_element_type=jnp.float32)
    squares = squares[:, :, 0].T.reshape(-1)
    summed, square_own = scattered(partial_value.astype(jnp.bfloat16), squares)
    mixed = (summed * lax.rsqrt(square_own / out_gain.shape[0] + EPSILON)[:, None]).astype(jnp.bfloat16)
    return (mixed, base_state)


def solution(mesh):
    placed = (
        P(("dp", "kv", "tp"), None),
        P(),
        P(None, ("kv", "tp")),
        P(None, ("kv", "tp")),
        P(None, ("kv", "tp")),
        P(None, ("kv", "tp")),
        P(),
        P(),
        P(),
        P(),
        P(),
        P(),
        P(),
        P(),
        P(("kv", "tp"), None),
        P("dp", ("kv", "tp"), None, None),
        P("dp", None, ("kv", "tp")),
        P("dp", None, ("kv", "tp")),
        P("dp", None, ("kv", "tp")),
        P("dp", None, ("kv", "tp")),
        P("dp"),
    )
    return jax.shard_map(
        body,
        mesh=mesh,
        in_specs=placed,
        out_specs=(P(("dp", "kv", "tp"), None), P("dp", ("kv", "tp"), None, None)),
        check_vma=False,
    )
```
